32 devices in a mesh: ep: 8 (over z, y), tp: 4 (over x, core).
Axes of the slice: x: 2, y: 2, z: 4, core: 2. Of those that a mesh axis runs over, the one named last changes fastest.
Arguments:
- query_rows: bfloat16 [4096, 1024], P('ep', 'tp'), may hold values from -60 to 60
- key_rows: bfloat16 [4096, 1024], P('ep', 'tp'), may hold values from -6 to 6
- value_rows: bfloat16 [4096, 1024], P('ep', 'tp'), may hold values from -6 to 6
- lambdas: float32 [8], P('tp'), may hold values from 0.3 to 0.8
- out_gain: float32 [128], replicated, may hold values from 0.1 to 1.9
- out_weight: bfloat16 [1024, 2048], P('tp'), may hold values from -0.1875 to 0.1875
- tokens: bfloat16 [4096, 2048], P(('ep', 'tp')), may hold values from -6 to 6
- norm_gain: float32 [2048], replicated, may hold values from 0.1 to 1.9
- group_ids: int32 [4096], P(('ep', 'tp')), may hold values from 0 to 3, as said below
- inner_ids: int32 [4096, 2], P(('ep', 'tp')), may hold values from 0 to 1, as said below
- route_weights: float32 [4096, 2], P(('ep', 'tp')), may hold values from 0.2 to 1
- gate_weight: bfloat16 [8, 2048, 1024], P('ep', None, 'tp'), may hold values from -0.125 to 0.125
- up_weight: bfloat16 [8, 2048, 1024], P('ep', None, 'tp'), may hold values from -0.125 to 0.125
- down_weight: bfloat16 [8, 1024, 2048], P('ep', 'tp'), may hold values from -0.1875 to 0.1875
Outputs:
- attended: bfloat16 [4096, 2048], P(('ep', 'tp'))
- combined: bfloat16 [4096, 2048], P(('ep', 'tp'))
The draws below stay inside these ranges and needn't reach their ends.
Inputs may be any that keep to these rules, and one draw needn't show every extreme that they name: In the 128 rows of one device no expert group_ids * 2 + inner_ids is named more than 40 times; some expert is named exactly 40 times in the rows of every device. `inner_ids`: the 2 entries of a row are different.
All inputs are finite; a program needn't handle non-finite values.
Results may differ from the reference program's by a relative error of at most 0.013.
Values may be sent and summed in bfloat16 or wider, within the bound.
A program may use at most 128 MiB of HBM per device.

```python
import jax
import jax.numpy as jnp
from jax import lax

D = 2048
HEADS = 8
DQ = 64
DV = 128
FF = 1024
GROUPS = 4
TOPK = 2
TOK_DEV = 128
SEG = 512
TOKENS = 4096
EXPERTS = 8
CAP = 40
N_EP = 8
N_TP = 4


def paired_scores(base_key):
    width_cols = HEADS * 2 * DQ
    query_base = jnp.clip(jax.random.normal(jax.random.fold_in(base_key, 21), (TOKENS, width_cols), jnp.float32), -4.5, 4.5) * 1.3
    key_base = jnp.clip(jax.random.normal(jax.random.fold_in(base_key, 22), (TOKENS, width_cols), jnp.float32), -4.5, 4.5) * 1.3
    return (query_base, key_base)


def draw_query_rows(key, part):
    return paired_scores(key)[0].astype(jnp.bfloat16)


def draw_key_rows(key, part):
    return paired_scores(key)[1].astype(jnp.bfloat16)


def route_cells(base_key):
    group_size = EXPERTS // GROUPS
    per_row = group_size // TOPK
    per_group = CAP * per_row
    blocks = TOKENS // TOK_DEV
    hot = jax.random.randint(jax.random.fold_in(base_key, 31), (), 0, GROUPS).astype(jnp.int32)

    def one_block(block_num):
        block_key = jax.random.fold_in(jax.random.fold_in(base_key, 32), block_num)
        spare = jax.random.permutation(jax.random.fold_in(block_key, 1), (GROUPS - 1) * per_group)
        spare = spare[:TOK_DEV - per_group].astype(jnp.int32)
        spare_group = spare // per_group
        spare_group = spare_group + (spare_group >= hot).astype(jnp.int32)
        cell_group = jnp.concatenate([jnp.zeros((per_group,), jnp.int32) + hot, spare_group])
        cell_local = jnp.concatenate([jnp.arange(per_group, dtype=jnp.int32), spare % per_group])
        order = jax.random.permutation(jax.random.fold_in(block_key, 2), TOK_DEV).astype(jnp.int32)
        tok_group = cell_group[order]
        tok_local = cell_local[order]
        row_of = tok_group * CAP + tok_local // per_row
        slot_num = tok_local % per_row
        scores = jax.random.randint(jax.random.fold_in(block_key, 3), (GROUPS * CAP, group_size), 0, 1 << 20)
        scores = scores * group_size + jnp.arange(group_size, dtype=jnp.int32)[None, :]
        shuffle = jnp.argsort(scores, axis=1).astype(jnp.int32)
        columns = slot_num[:, None] * TOPK + jnp.arange(TOPK, dtype=jnp.int32)[None, :]
        chosen = jnp.take_along_axis(shuffle[row_of], columns, axis=1)
        return (tok_group, chosen)
    groups_all, inner_all = jax.vmap(one_block)(jnp.arange(blocks, dtype=jnp.int32))
    return (groups_all.reshape(TOKENS).astype(jnp.int32), inner_all.reshape(TOKENS, TOPK).astype(jnp.int32))


def draw_group_ids(key, part):
    return route_cells(key)[0]


def draw_inner_ids(key, part):
    return route_cells(key)[1]


def level_of(stream_key, shape, split, least, top_value):
    level, own = 1.0, jax.random.fold_in(stream_key, 6)
    for axis_at, parts in split:
        draws = jnp.exp(jax.random.uniform(jax.random.fold_in(own, axis_at), (parts,), jnp.float32, least / len(split), top_value / len(split)))
        level = level * jnp.repeat(draws, shape[axis_at] // parts).reshape([-1 if axis == axis_at else 1 for axis in range(len(shape))])
    return level


def normal_values(stream_key, extent, scale, bound, cuts=(), kind=jnp.bfloat16):
    values = jax.random.normal(stream_key, extent, jnp.float32) * scale
    if len(cuts) > 0:
        values = level_of(stream_key, extent, cuts, -0.22, 0.18) * values
    return jnp.clip(values, min=-bound, max=bound).astype(kind)


def setup_inputs(seed: int = 0) -> dict:
    keys = jax.random.split(jax.random.key(seed), 15)
    query_rows = draw_query_rows(jax.random.fold_in(keys[14], 71), 0)
    key_rows = draw_key_rows(jax.random.fold_in(keys[14], 71), 0)
    value_rows = normal_values(keys[2], (TOKENS, HEADS * DV), 1.0, 6.0, ((0, 8), (1, 4)))
    lambdas = jnp.clip(0.3 + 0.5 * jax.random.uniform(keys[3], (HEADS,), jnp.float32) ** level_of(keys[3], (HEADS,), ((0, 4),), -0.2, 0.2), 0.3, 0.8)
    out_gain = jnp.clip(1.0 + 0.18 * jax.random.normal(keys[4], (DV,), jnp.float32), 0.1, 1.9)
    out_weight = normal_values(keys[5], (HEADS * DV, D), (HEADS * DV) ** -0.5, 0.1875, ((0, 4),))
    tokens = normal_values(keys[6], (TOKENS, D), 1.0, 6.0, ((0, 32),))
    norm_gain = jnp.clip(1.0 + 0.18 * jax.random.normal(keys[7], (D,), jnp.float32), 0.1, 1.9)
    group_ids = draw_group_ids(jax.random.fold_in(keys[14], 71), 0)
    inner_ids = draw_inner_ids(jax.random.fold_in(keys[14], 71), 0)
    route_weights = jnp.clip(0.2 + 0.8 * jax.random.uniform(keys[10], (TOKENS, TOPK), jnp.float32) ** level_of(keys[10], (TOKENS, TOPK), ((0, 32),), -0.2, 0.2), 0.2, 1.0)
    gate_weight = normal_values(keys[11], (EXPERTS, D, FF), D ** -0.5, 0.125, ((0, 8), (2, 4)))
    up_weight = normal_values(keys[12], (EXPERTS, D, FF), D ** -0.5, 0.125, ((0, 8), (2, 4)))
    down_weight = normal_values(keys[13], (EXPERTS, FF, D), FF ** -0.5, 0.1875, ((0, 8), (1, 4)))
    return dict(query_rows=query_rows, key_rows=key_rows, value_rows=value_rows, lambdas=lambdas, out_gain=out_gain, out_weight=out_weight, tokens=tokens, norm_gain=norm_gain, group_ids=group_ids, inner_ids=inner_ids, route_weights=route_weights, gate_weight=gate_weight, up_weight=up_weight, down_weight=down_weight)


eps = 1e-06

def one_map(query_part, key_all, value_all, allowed):
    scores = jnp.dot(query_part, key_all.T, preferred_element_type=jnp.float32) * DQ ** (-0.5)
    scores = jnp.where(allowed, scores, -jnp.inf)
    row_top = lax.optimization_barrier(jnp.max(scores, axis=1, keepdims=True))
    exps = jnp.exp(scores - row_top)
    totals = lax.optimization_barrier(jnp.sum(exps, axis=1, keepdims=True))
    weighted = jnp.dot(exps.astype(jnp.bfloat16), value_all, preferred_element_type=jnp.float32)
    return weighted / totals

def head_output(operands):
    query_head, key_head, value_head, lambda_head = operands
    key_pos = jnp.arange(TOKENS, dtype=jnp.int32)

    def query_block(block_num):
        first_row = block_num * SEG
        query_part = lax.dynamic_slice_in_dim(query_head, first_row, SEG, 0)
        query_pos = first_row + jnp.arange(SEG, dtype=jnp.int32)
        allowed = key_pos[None, :] <= query_pos[:, None]
        first_map = one_map(query_part[:, 0], key_head[:, 0], value_head, allowed)
        second_map = one_map(query_part[:, 1], key_head[:, 1], value_head, allowed)
        heads_out = first_map - lambda_head * second_map
        mean_sq = lax.optimization_barrier(jnp.mean(heads_out * heads_out, axis=1, keepdims=True))
        return heads_out * lax.rsqrt(mean_sq + eps)
    return lax.map(query_block, jnp.arange(N_EP, dtype=jnp.int32)).reshape(TOKENS, DV)

def reference(query_rows, key_rows, value_rows, lambdas, out_gain, out_weight, tokens, norm_gain, group_ids, inner_ids, route_weights, gate_weight, up_weight, down_weight):
    query_heads = query_rows.reshape(TOKENS, HEADS, 2, DQ).transpose(1, 0, 2, 3)
    key_heads = key_rows.reshape(TOKENS, HEADS, 2, DQ).transpose(1, 0, 2, 3)
    value_heads = value_rows.reshape(TOKENS, HEADS, DV).transpose(1, 0, 2)
    per_head = lax.map(head_output, (query_heads, key_heads, value_heads, lambdas))
    normed_heads = (per_head * out_gain).astype(jnp.bfloat16).transpose(1, 0, 2).reshape(TOKENS, HEADS * DV)
    attended = jnp.dot(normed_heads, out_weight, preferred_element_type=jnp.float32).astype(jnp.bfloat16)
    tok_wide = tokens.astype(jnp.float32)
    normed = (tok_wide * lax.rsqrt(lax.optimization_barrier(jnp.mean(tok_wide * tok_wide, axis=1, keepdims=True)) + eps) * norm_gain).astype(jnp.bfloat16)
    picks = (group_ids[:, None] * (EXPERTS // GROUPS) + inner_ids).reshape(-1)
    flat_weights = route_weights.reshape(-1)
    room = N_EP * N_TP * CAP

    def one_expert(running, expert_num):
        matches = picks == expert_num
        picked = jnp.nonzero(matches, size=room, fill_value=0)[0].astype(jnp.int32)
        live = jnp.arange(room) < jnp.sum(matches)
        token_ids = picked // TOPK
        chosen_rows = normed[token_ids]
        gate_pre = jnp.dot(chosen_rows, gate_weight[expert_num], preferred_element_type=jnp.float32)
        up_pre = jnp.dot(chosen_rows, up_weight[expert_num], preferred_element_type=jnp.float32)
        hidden = (jax.nn.silu(gate_pre) * up_pre).astype(jnp.bfloat16)
        result = jnp.dot(hidden, down_weight[expert_num], preferred_element_type=jnp.float32).astype(jnp.bfloat16)
        weight_col = jnp.where(live, flat_weights[picked], jnp.float32(0.0))
        running = running.at[token_ids].add(result.astype(jnp.float32) * weight_col[:, None])
        return (running, None)
    running, _ = lax.scan(one_expert, jnp.zeros((TOKENS, D), jnp.float32), jnp.arange(EXPERTS, dtype=jnp.int32))
    combined = running.astype(jnp.bfloat16)
    return (attended, combined)
```

```python
import functools

import jax
import jax.numpy as jnp
from jax import lax
from jax.experimental import pallas as pl
from jax.experimental.pallas import tpu as pltpu
from jax.sharding import PartitionSpec as P

GROUPS = 4

eps = 1e-06
neg_big = -1e30
f32, bf16 = jnp.float32, jnp.bfloat16


def swap(value, axis, mask):
    count = lax.axis_size(axis)
    return lax.ppermute(value, axis, [(i, i ^ mask) for i in range(count)])


def flash_kernel(seg_rows, rows_seg, sub_rows, segs, offset_ref, lambda_ref, gain_ref, q_ref, k_ref, v_ref, o_ref):
    tile = pl.program_id(0)
    rows = segs * rows_seg
    keys = segs * seg_rows
    width = v_ref.shape[1]
    lane = lax.broadcasted_iota(jnp.int32, (rows, width), 1)
    queries = q_ref[...] * jnp.asarray((width // 2) ** (-0.5), bf16)
    zero = jnp.zeros_like(queries)
    stacked = jnp.concatenate(
        [jnp.where(lane < width // 2, queries, zero), jnp.where(lane < width // 2, zero, queries)], axis=0
    )

    def block(number, state, masked):
        top, total, accum = state
        start = pl.multiple_of(number * keys, keys)
        scores = lax.dot_general(
            stacked, k_ref[pl.ds(start, keys), :], (((1,), (1,)), ((), ())), preferred_element_type=f32
        )
        if masked:
            row = lax.broadcasted_iota(jnp.int32, (rows, keys), 0)
            key = lax.broadcasted_iota(jnp.int32, (rows, keys), 1)
            part = row // sub_rows
            position = part * (seg_rows * sub_rows // rows_seg) + row % sub_rows + offset_ref[0]
            allowed = key <= position
            allowed = jnp.concatenate([allowed, allowed], axis=0)
            scores = jnp.where(allowed, scores, neg_big)
        top_new = jnp.maximum(top, jnp.max(scores, axis=1, keepdims=True))
        exps = jnp.exp(scores - top_new)
        fade = jnp.exp(top - top_new)
        total = total * fade + jnp.sum(exps, axis=1, keepdims=True)
        accum = accum * fade + jnp.dot(
            exps.astype(bf16), v_ref[pl.ds(start, keys), :], preferred_element_type=f32
        )
        return top_new, total, accum

    state = (
        jnp.full((2 * rows, 1), neg_big, f32),
        jnp.zeros((2 * rows, 1), f32),
        jnp.zeros((2 * rows, width), f32),
    )
    state = block(tile, state, True)
    state = lax.fori_loop(0, tile, lambda number, inner: block(number, inner, False), state)
    top, total, accum = state
    out = accum / total
    out = out[:rows] - lambda_ref[0] * out[rows:]
    mean_sq = jnp.mean(out * out, axis=1, keepdims=True)
    o_ref[...] = (out * lax.rsqrt(mean_sq + eps) * gain_ref[...]).astype(bf16)


def flash(queries, keys, values, offset, lambda_head, gain, seg_rows, sub_rows):
    total_rows, width = queries.shape
    segments = keys.shape[0] // seg_rows
    rows_seg = total_rows // segments
    segs = 2 if segments % 2 == 0 else 1
    tiles = segments // segs
    rows = segs * rows_seg
    whole = lambda shape: pl.BlockSpec(shape, lambda i: (0, 0))
    return pl.pallas_call(
        functools.partial(flash_kernel, seg_rows, rows_seg, sub_rows, segs),
        grid=(tiles,),
        in_specs=[
            pl.BlockSpec(memory_space=pltpu.SMEM),
            pl.BlockSpec(memory_space=pltpu.SMEM),
            whole((1, width)),
            pl.BlockSpec((rows, width), lambda i: (i, 0)),
            whole(keys.shape),
            whole(values.shape),
        ],
        out_specs=pl.BlockSpec((rows, width), lambda i: (i, 0)),
        out_shape=jax.ShapeDtypeStruct((total_rows, width), bf16),
        cost_estimate=pl.CostEstimate(
            flops=4 * total_rows * keys.shape[0] * width,
            bytes_accessed=4 * keys.size,
            transcendentals=total_rows * keys.shape[0],
        ),
        name="attend",
    )(offset, lambda_head, gain, queries, keys, values)


def body(
    query_rows,
    key_rows,
    value_rows,
    lambdas,
    out_gain,
    out_weight,
    tokens,
    norm_gain,
    group_ids,
    inner_ids,
    route_weights,
    gate_weight,
    up_weight,
    down_weight,
):
    seg_rows = query_rows.shape[0]
    heads_here = lambdas.shape[0]
    width = out_gain.shape[0]
    tok_dev, model_width = tokens.shape
    topk_count = inner_ids.shape[1]
    n_ep, n_tp = lax.axis_size("ep"), lax.axis_size("tp")
    ep_index, tp_index = lax.axis_index("ep"), lax.axis_index("tp")
    core, side = tp_index % 2, tp_index // 2
    group_size = n_ep // GROUPS
    capacity = 5 * tok_dev * topk_count // (4 * n_ep)
    room = capacity * group_size // topk_count

    tok_wide = tokens.astype(f32)
    normed = (
        tok_wide * lax.rsqrt(jnp.mean(tok_wide * tok_wide, axis=1, keepdims=True) + eps) * norm_gain
    ).astype(bf16)
    in_group = group_ids[:, None] == jnp.arange(GROUPS, dtype=jnp.int32)[None, :]
    earlier = jnp.tril(jnp.ones((tok_dev, tok_dev), f32), -1)
    rank = jnp.sum(jnp.dot(earlier, in_group.astype(f32)) * in_group, axis=1).astype(jnp.int32)
    slot_of = group_ids * room + rank
    placing = slot_of[:, None] == jnp.arange(GROUPS * room, dtype=jnp.int32)[None, :]
    place = placing.astype(bf16)
    expert_label = jnp.arange(group_size, dtype=jnp.int32)
    weight_of = jnp.sum(
        jnp.where(inner_ids[:, :, None] == expert_label[None, None, :], route_weights[:, :, None], 0.0), axis=1
    )
    high = lax.reduce_precision(weight_of, 8, 7)
    middle = lax.reduce_precision(weight_of - high, 8, 7)
    low = weight_of - high - middle
    thirds = jnp.concatenate([high, middle, low], axis=1)
    thirds = jnp.pad(thirds, ((0, 0), (0, 128 - 3 * group_size))).astype(bf16)
    wide = jnp.concatenate([normed, thirds], axis=1)
    outgoing = jnp.einsum("ts,td->sd", place, wide, preferred_element_type=f32).astype(bf16)
    lines = [[g * group_size + y for g in range(GROUPS)] for y in range(group_size)]
    own = lax.all_to_all(outgoing, "ep", 0, 0, axis_index_groups=lines, tiled=True)

    half = seg_rows // 2
    pair_heads = 2 * heads_here
    ways = n_ep // pair_heads
    sub = half // 2 // ways
    split = lambda rows: rows.reshape(2, half, heads_here, width).transpose(0, 2, 1, 3)
    packed = jnp.concatenate([split(key_rows), split(value_rows), split(query_rows)], axis=2)
    kept = lax.dynamic_index_in_dim(packed, core, 0, keepdims=False)
    given = lax.dynamic_index_in_dim(packed, 1 - core, 0, keepdims=False)
    other = swap(given, "tp", 1)
    in_order = lambda a, b, axis: jnp.where(
        core == 0, jnp.concatenate([a, b], axis=axis), jnp.concatenate([b, a], axis=axis)
    )
    heads = in_order(kept, other, 0)
    key_value = jnp.broadcast_to(
        heads[:, None, : 2 * half], (pair_heads, ways, 2 * half, width)
    )
    query_part = (
        heads[:, 2 * half :].reshape(pair_heads, 2, ways, sub, width).transpose(0, 2, 1, 3, 4)
    ).reshape(pair_heads, ways, 2 * sub, width)
    sent = jnp.concatenate([key_value, query_part], axis=2).reshape(n_ep, 2 * half + 2 * sub, width)
    arrived = lax.all_to_all(sent, "ep", 0, 0, tiled=True)
    query_got = arrived[:, 2 * half :].reshape(n_ep, 2, sub, width)
    query_kept = lax.dynamic_index_in_dim(query_got, core, 1, keepdims=False)
    query_given = lax.dynamic_index_in_dim(query_got, 1 - core, 1, keepdims=False)
    near = jnp.concatenate([arrived[:, : 2 * half], query_kept], axis=1)
    far = swap(jnp.concatenate([arrived[:, : 2 * half], query_given], axis=1), "tp", 1)
    keys = in_order(near[:, :half], far[:, :half], 1).reshape(n_ep * seg_rows, width)
    values = in_order(near[:, half : 2 * half], far[:, half : 2 * half], 1).reshape(n_ep * seg_rows, width)
    queries = in_order(near[:, 2 * half :], far[:, 2 * half :], 1).reshape(n_ep * 2 * sub, width)
    pair_lambdas = in_order(lambdas, swap(lambdas, "tp", 1), 0)
    pair_weight = in_order(out_weight, swap(out_weight, "tp", 1), 0)
    offset = (core * (half // 2) + (ep_index % ways) * sub).astype(jnp.int32).reshape(1)
    lambda_head = lax.dynamic_slice_in_dim(pair_lambdas, ep_index // ways, 1, 0)
    head_rows = flash(
        queries, keys, values, offset, lambda_head, out_gain.reshape(1, width), seg_rows, sub
    )
    came = lax.all_to_all(head_rows.reshape(n_ep, 2 * sub, width), "ep", 0, 0, tiled=True)
    came = came.reshape(pair_heads, ways, 2, sub, width).transpose(2, 1, 3, 0, 4)
    came = came.reshape(2, ways * sub, pair_heads * width)
    came_far = lax.dynamic_index_in_dim(came, 1 - side, 0, keepdims=False)
    came_near = lax.dynamic_index_in_dim(came, side, 0, keepdims=False)
    part_far = jnp.dot(came_far, pair_weight, preferred_element_type=f32).astype(bf16)
    part_near = jnp.dot(came_near, pair_weight, preferred_element_type=f32)
    attended = (part_near + swap(part_far, "tp", 2).astype(f32)).astype(bf16)

    rows_own = own.shape[0]
    cut = rows_own // 2 // 16 * 16
    over_x = swap(own, "tp", 2)
    over_y = swap(own, "ep", 1)
    both = jnp.concatenate([swap(over_x[:cut], "ep", 1), swap(over_y[cut:], "tp", 2)], axis=0)
    blocks = [own, over_x, over_y, both]
    blocks = blocks + [swap(block, "tp", 1) for block in blocks]
    mask = 2
    while mask < group_size:
        blocks = blocks + [swap(block, "ep", mask) for block in blocks]
        mask *= 2
    gathered = jnp.concatenate(blocks, axis=0)
    rows_in = gathered[:, :model_width]
    tail = gathered[:, model_width:].astype(f32)
    label = ep_index % group_size
    lane = jnp.arange(tail.shape[1], dtype=jnp.int32)
    mine = (lane < 3 * group_size) & (lane % group_size == label)
    row_weight = jnp.sum(jnp.where(mine[None, :], tail, 0.0), axis=1, keepdims=True)
    gate_pre = jnp.dot(rows_in, gate_weight[0], preferred_element_type=f32)
    up_pre = jnp.dot(rows_in, up_weight[0], preferred_element_type=f32)
    hidden = (jax.nn.silu(gate_pre) * up_pre).astype(bf16)

    count = len(blocks)
    result = (jnp.dot(hidden, down_weight[0], preferred_element_type=f32) * row_weight).astype(bf16)
    sums = [result[i * rows_own : (i + 1) * rows_own] for i in range(count)]
    add = lambda a, b: (a.astype(f32) + b.astype(f32)).astype(bf16)
    while mask > 2:
        mask //= 2
        middle_at = len(sums) // 2
        sums = [add(a, swap(b, "ep", mask)) for a, b in zip(sums[:middle_at], sums[middle_at:])]
    sums = [add(a, swap(b, "tp", 1)) for a, b in zip(sums[:4], sums[4:])]
    from_y = swap(sums[3][:cut], "ep", 1)
    from_x = swap(sums[3][cut:], "tp", 2)
    for_x = jnp.concatenate([add(sums[1][:cut], from_y), sums[1][cut:]], axis=0)
    for_y = jnp.concatenate([sums[2][:cut], add(sums[2][cut:], from_x)], axis=0)
    total = (
        sums[0].astype(f32) + swap(for_x, "tp", 2).astype(f32) + swap(for_y, "ep", 1).astype(f32)
    ).astype(bf16)
    returned = lax.all_to_all(total, "ep", 0, 0, axis_index_groups=lines, tiled=True)
    combined = jnp.dot(place, returned, preferred_element_type=f32).astype(bf16)
    return (attended, combined)


def solution(mesh):
    in_specs = (
        P("ep", "tp"),
        P("ep", "tp"),
        P("ep", "tp"),
        P("tp"),
        P(),
        P("tp", None),
        P(("ep", "tp"), None),
        P(),
        P(("ep", "tp")),
        P(("ep", "tp"), None),
        P(("ep", "tp"), None),
        P("ep", None, "tp"),
        P("ep", None, "tp"),
        P("ep", "tp", None),
    )
    out_specs = (P(("ep", "tp"), None), P(("ep", "tp"), None))
    return jax.shard_map(body, mesh=mesh, in_specs=in_specs, out_specs=out_specs, check_vma=False)
```

```python
import functools

import jax
import jax.numpy as jnp
from jax import lax
from jax.experimental import pallas as pl
from jax.experimental.pallas import tpu as pltpu
from jax.sharding import PartitionSpec as P


GROUPS = 4

eps = 1e-06
neg_big = -1e30
f32, bf16 = jnp.float32, jnp.bfloat16


def swap(value, axis, mask):
    count = lax.axis_size(axis)
    return lax.ppermute(value, axis, [(i, i ^ mask) for i in range(count)])


def flash_kernel(seg_rows, rows_seg, sub_rows, segs, first, offset_ref, lambda_ref, gain_ref, q_ref, k_ref, v_ref, o_ref):
    tile = pl.program_id(0) + first
    rows = segs * rows_seg
    keys = segs * seg_rows
    width = v_ref.shape[1]
    lane = lax.broadcasted_iota(jnp.int32, (rows, width), 1)
    queries = q_ref[...] * jnp.asarray((width // 2) ** (-0.5), bf16)
    zero = jnp.zeros_like(queries)
    stacked = jnp.concatenate(
        [jnp.where(lane < width // 2, queries, zero), jnp.where(lane < width // 2, zero, queries)], axis=0
    )

    def block(number, state, masked):
        top, total, accum = state
        start = pl.multiple_of(number * keys, keys)
        scores = lax.dot_general(
            stacked, k_ref[pl.ds(start, keys), :], (((1,), (1,)), ((), ())), preferred_element_type=f32
        )
        if masked:
            row = lax.broadcasted_iota(jnp.int32, (rows, keys), 0)
            key = lax.broadcasted_iota(jnp.int32, (rows, keys), 1)
            part = row // sub_rows
            position = part * (seg_rows * sub_rows // rows_seg) + row % sub_rows + offset_ref[0]
            allowed = key <= position
            allowed = jnp.concatenate([allowed, allowed], axis=0)
            scores = jnp.where(allowed, scores, neg_big)
        top_new = jnp.maximum(top, jnp.max(scores, axis=1, keepdims=True))
        exps = jnp.exp(scores - top_new)
        fade = jnp.exp(top - top_new)
        total = total * fade + jnp.sum(exps, axis=1, keepdims=True)
        accum = accum * fade + jnp.dot(
            exps.astype(bf16), v_ref[pl.ds(start, keys), :], preferred_element_type=f32
        )
        return top_new, total, accum

    state = (
        jnp.full((2 * rows, 1), neg_big, f32),
        jnp.zeros((2 * rows, 1), f32),
        jnp.zeros((2 * rows, width), f32),
    )
    state = block(tile, state, True)
    state = lax.fori_loop(0, tile, lambda number, inner: block(number, inner, False), state)
    _, total, accum = state
    out = accum / total
    out = out[:rows] - lambda_ref[0] * out[rows:]
    mean_sq = jnp.mean(out * out, axis=1, keepdims=True)
    o_ref[...] = (out * lax.rsqrt(mean_sq + eps) * gain_ref[...]).astype(bf16)


def flash(queries, keys, values, offset, lambda_head, gain, seg_rows, sub_rows):
    total_rows, width = queries.shape
    segments = keys.shape[0] // seg_rows
    rows_seg = total_rows // segments
    segs = 2 if segments % 2 == 0 else 1
    tiles = segments // segs
    rows = segs * rows_seg
    whole = lambda shape: pl.BlockSpec(shape, lambda i: (0, 0))
    cut = tiles * 3 // 4
    parts = []
    for first, count in ((0, cut), (cut, tiles - cut)):
        parts.append(
            pl.pallas_call(
                functools.partial(flash_kernel, seg_rows, rows_seg, sub_rows, segs, first),
                grid=(count,),
                in_specs=[
                    pl.BlockSpec(memory_space=pltpu.SMEM),
                    pl.BlockSpec(memory_space=pltpu.SMEM),
                    whole((1, width)),
                    pl.BlockSpec((rows, width), lambda i, first=first: (i + first, 0)),
                    whole(keys.shape),
                    whole(values.shape),
                ],
                out_specs=pl.BlockSpec((rows, width), lambda i: (i, 0)),
                out_shape=jax.ShapeDtypeStruct((count * rows, width), bf16),
                cost_estimate=pl.CostEstimate(
                    flops=2 * total_rows * keys.shape[0] * width,
                    bytes_accessed=4 * keys.size,
                    transcendentals=total_rows * keys.shape[0] // 2,
                ),
                compiler_params=pltpu.CompilerParams(vmem_limit_bytes=32 * 2**20),
            )(offset, lambda_head, gain, queries, keys, values)
        )
    return jnp.concatenate(parts, axis=0)


def expert_kernel(group_size, label_ref, near_ref, far_ref, gate_ref, up_ref, down_ref, near_out, far_out):
    width = gate_ref.shape[0]
    count = near_ref.shape[0]
    both = jnp.concatenate([near_ref[...], far_ref[...]], axis=0)
    rows = both[:, :width]
    tail = both[:, width:].astype(f32)
    lane = lax.broadcasted_iota(jnp.int32, tail.shape, 1)
    mine = (lane < 3 * group_size) & (lane % group_size == label_ref[0])
    row_weight = jnp.sum(jnp.where(mine, tail, 0.0), axis=1, keepdims=True)
    gate_pre = jnp.dot(rows, gate_ref[...], preferred_element_type=f32)
    up_pre = jnp.dot(rows, up_ref[...], preferred_element_type=f32)
    hidden = (gate_pre / (1.0 + jnp.exp(-gate_pre)) * up_pre).astype(bf16)
    out = (jnp.dot(hidden, down_ref[...], preferred_element_type=f32) * row_weight).astype(bf16)
    near_out[...] = out[:count]
    far_out[...] = out[count:]


def expert(near, far, label, gate, up, down, group_size):
    rows = near.shape[0]
    vmem = pl.BlockSpec(memory_space=pltpu.VMEM)
    return pl.pallas_call(
        functools.partial(expert_kernel, group_size),
        in_specs=[pl.BlockSpec(memory_space=pltpu.SMEM)] + [vmem] * 5,
        out_specs=[vmem, vmem],
        out_shape=[jax.ShapeDtypeStruct((rows, down.shape[1]), bf16)] * 2,
        cost_estimate=pl.CostEstimate(
            flops=12 * rows * gate.size, bytes_accessed=6 * gate.size, transcendentals=2 * rows * gate.shape[1]
        ),
        compiler_params=pltpu.CompilerParams(vmem_limit_bytes=20 * 2**20),
        name="expert",
    )(label, near, far, gate, up, down)


def layer(
    query_rows,
    key_rows,
    value_rows,
    lambdas,
    out_gain,
    out_weight,
    tokens,
    norm_gain,
    group_ids,
    inner_ids,
    route_weights,
    gate_weight,
    up_weight,
    down_weight,
):
    seg_rows = query_rows.shape[0]
    heads_here = lambdas.shape[0]
    width = out_gain.shape[0]
    tok_dev, _ = tokens.shape
    topk_count = inner_ids.shape[1]
    n_ep = lax.axis_size("ep")
    ep_index, tp_index = lax.axis_index("ep"), lax.axis_index("tp")
    core, side = tp_index % 2, tp_index // 2
    group_size = n_ep // GROUPS
    capacity = 5 * tok_dev * topk_count // (4 * n_ep)
    room = capacity * group_size // topk_count

    tok_wide = tokens.astype(f32)
    normed = (
        tok_wide * lax.rsqrt(jnp.mean(tok_wide * tok_wide, axis=1, keepdims=True) + eps) * norm_gain
    ).astype(bf16)
    in_group = group_ids[:, None] == jnp.arange(GROUPS, dtype=jnp.int32)[None, :]
    earlier = jnp.tril(jnp.ones((tok_dev, tok_dev), f32), -1)
    rank = jnp.sum(jnp.dot(earlier, in_group.astype(f32)) * in_group, axis=1).astype(jnp.int32)
    slot_of = (group_ids ^ (ep_index // group_size)) * room + rank
    placing = slot_of[:, None] == jnp.arange(GROUPS * room, dtype=jnp.int32)[None, :]
    place = placing.astype(bf16)
    expert_label = jnp.arange(group_size, dtype=jnp.int32)
    weight_of = jnp.sum(
        jnp.where(inner_ids[:, :, None] == expert_label[None, None, :], route_weights[:, :, None], 0.0), axis=1
    )
    high = lax.reduce_precision(weight_of, 8, 7)
    middle = lax.reduce_precision(weight_of - high, 8, 7)
    low = weight_of - high - middle
    thirds = jnp.concatenate([high, middle, low], axis=1)
    thirds = jnp.pad(thirds, ((0, 0), (0, 128 - 3 * group_size))).astype(bf16)
    wide = jnp.concatenate([normed, thirds], axis=1)
    outgoing = jnp.einsum("ts,td->sd", place, wide, preferred_element_type=f32).astype(bf16)
    block_of = lambda rows, diff: rows[diff * room : (diff + 1) * room]
    came_in = [swap(block_of(outgoing, diff), "ep", diff * group_size) for diff in range(1, GROUPS)]
    own = jnp.concatenate([block_of(outgoing, 0)] + came_in, axis=0)

    half = seg_rows // 2
    pair_heads = 2 * heads_here
    ways = n_ep // pair_heads
    sub = half // 2 // ways

    def packed(index):
        start = index * half
        parts = [lax.dynamic_slice_in_dim(rows, start, half, 0) for rows in (key_rows, value_rows, query_rows)]
        by_head = [
            jnp.concatenate([part[:, j * width : (j + 1) * width] for part in parts], axis=0)
            for j in range(heads_here)
        ]
        return jnp.stack(by_head, axis=0)

    kept, given = packed(core), packed(1 - core)
    other = swap(given, "tp", 1)
    in_order = lambda a, b, axis: jnp.where(
        core == 0, jnp.concatenate([a, b], axis=axis), jnp.concatenate([b, a], axis=axis)
    )
    heads = in_order(kept, other, 0)
    key_value = jnp.broadcast_to(
        heads[:, None, : 2 * half], (pair_heads, ways, 2 * half, width)
    )
    query_part = (
        heads[:, 2 * half :].reshape(pair_heads, 2, ways, sub, width).transpose(0, 2, 1, 3, 4)
    ).reshape(pair_heads, ways, 2 * sub, width)
    sent = jnp.concatenate([key_value, query_part], axis=2)
    sent = sent.reshape(n_ep, 2 * half + 2 * sub, width)
    arrived = lax.all_to_all(sent, "ep", 0, 0, tiled=True)
    query_got = arrived[:, 2 * half :].reshape(n_ep, 2, sub, width)
    query_kept = lax.dynamic_index_in_dim(query_got, core, 1, keepdims=False)
    query_given = lax.dynamic_index_in_dim(query_got, 1 - core, 1, keepdims=False)
    near = jnp.concatenate([arrived[:, : 2 * half], query_kept], axis=1)
    far = jnp.concatenate([arrived[:, : 2 * half], query_given], axis=1)
    far = swap(far, "tp", 1)
    keys = in_order(near[:, :half], far[:, :half], 1).reshape(n_ep * seg_rows, width)
    values = in_order(near[:, half : 2 * half], far[:, half : 2 * half], 1).reshape(n_ep * seg_rows, width)
    queries = in_order(near[:, 2 * half :], far[:, 2 * half :], 1).reshape(n_ep * 2 * sub, width)
    pair_lambdas = in_order(lambdas, swap(lambdas, "tp", 1), 0)
    far_weight = swap(out_weight, "tp", 2)
    weight_parts = [out_weight, swap(out_weight, "tp", 1), far_weight, swap(far_weight, "tp", 1)]
    offset = (core * (half // 2) + (ep_index % ways) * sub).astype(jnp.int32).reshape(1)
    lambda_head = lax.dynamic_slice_in_dim(pair_lambdas, ep_index // ways, 1, 0)
    head_rows = flash(
        queries, keys, values, offset, lambda_head, out_gain.reshape(1, width), seg_rows, sub
    )
    came = lax.all_to_all(head_rows.reshape(n_ep, 2 * sub, width), "ep", 0, 0, tiled=True)
    came = came.reshape(pair_heads, ways, 2, sub, width).transpose(2, 0, 1, 3, 4)
    came = came.reshape(2, pair_heads, ways * sub, width)
    came_far = lax.dynamic_index_in_dim(came, 1 - side, 0, keepdims=False)
    came_near = lax.dynamic_index_in_dim(came, side, 0, keepdims=False)
    came_side = swap(came_far, "tp", 2)
    attended = 0.0
    for number, heads_part in enumerate((came_near, came_side)):
        for step in range(2):
            first = (core if step == 0 else 1 - core) * heads_here
            some = lax.dynamic_slice_in_dim(heads_part, first, heads_here, 0)
            some = some.transpose(1, 0, 2).reshape(ways * sub, heads_here * width)
            attended += jnp.dot(some, weight_parts[2 * number + step], preferred_element_type=f32)
    attended = attended.astype(bf16)

    rows_own = own.shape[0]
    cut = rows_own // 2 // 16 * 16
    over_x = swap(own, "tp", 2)
    over_y = swap(own, "ep", 1)
    both = swap(over_y, "tp", 2)
    near_blocks = [own, over_x, over_y, both]
    far_blocks = [swap(block, "tp", 1) for block in near_blocks]
    mask = 2
    while mask < group_size:
        near_blocks = near_blocks + [swap(block, "ep", mask) for block in near_blocks]
        far_blocks = far_blocks + [swap(block, "ep", mask) for block in far_blocks]
        mask *= 2
    label = (ep_index % group_size).astype(jnp.int32).reshape(1)
    results = []
    for near, far in zip(near_blocks, far_blocks):
        results.append(
            expert(near, far, label, gate_weight[0], up_weight[0], down_weight[0], group_size)
        )
    add = lambda a, b: (a.astype(f32) + b.astype(f32)).astype(bf16)
    sums = [add(near, swap(far, "tp", 1)) for near, far in results]
    while mask > 2:
        mask //= 2
        middle_at = len(sums) // 2
        sums = [add(a, swap(b, "ep", mask)) for a, b in zip(sums[:middle_at], sums[middle_at:])]
    from_y = swap(sums[3][:cut], "ep", 1)
    from_x = swap(sums[3][cut:], "tp", 2)
    for_x = jnp.concatenate([add(sums[1][:cut], from_y), sums[1][cut:]], axis=0)
    for_y = jnp.concatenate([sums[2][:cut], add(sums[2][cut:], from_x)], axis=0)
    got_x = swap(for_x, "tp", 2)
    got_y = swap(for_y, "ep", 1)
    total = (sums[0].astype(f32) + got_x.astype(f32) + got_y.astype(f32)).astype(bf16)
    came_back = [swap(block_of(total, diff), "ep", diff * group_size) for diff in range(1, GROUPS)]
    returned = jnp.concatenate([block_of(total, 0)] + came_back, axis=0)
    combined = jnp.dot(place, returned, preferred_element_type=f32).astype(bf16)
    return (attended, combined)


def solution(mesh):
    in_specs = (
        P("ep", "tp"),
        P("ep", "tp"),
        P("ep", "tp"),
        P("tp"),
        P(),
        P("tp", None),
        P(("ep", "tp"), None),
        P(),
        P(("ep", "tp")),
        P(("ep", "tp"), None),
        P(("ep", "tp"), None),
        P("ep", None, "tp"),
        P("ep", None, "tp"),
        P("ep", "tp", None),
    )
    out_specs = (P(("ep", "tp"), None), P(("ep", "tp"), None))
    return jax.shard_map(layer, mesh=mesh, in_specs=in_specs, out_specs=out_specs, check_vma=False)
```
